256 devices in a mesh: sp: 32 (over z, x), tp: 8 (over y, core).
Axes of the slice: x: 4, y: 4, z: 8, core: 2. Of those that a mesh axis runs over, the one named last changes fastest.
Arguments:
- tokens: bfloat16 [12288, 2048], P('sp', 'tp'), may hold values from -6 to 6
- ret_query: bfloat16 [2048, 1024], P(None, 'tp'), may hold values from -0.125 to 0.125
- ret_key: bfloat16 [2048, 1024], P(None, 'tp'), may hold values from -0.125 to 0.125
- ret_value: bfloat16 [2048, 1024], P(None, 'tp'), may hold values from -0.125 to 0.125
- stick_query: bfloat16 [2048, 1024], P(None, 'tp'), may hold values from -0.125 to 0.125
- stick_key: bfloat16 [2048, 1024], P(None, 'tp'), may hold values from -0.125 to 0.125
- stick_value: bfloat16 [2048, 1024], P(None, 'tp'), may hold values from -0.125 to 0.125
- log_decay: float32 [12288, 8], P('sp', 'tp'), may hold values from -1.2 to 0
- stick_bias: float32 [8], P('tp'), may hold values from -13 to -5
- out_ret: bfloat16 [1024, 2048], P('tp'), may hold values from -0.125 to 0.125
- out_stick: bfloat16 [1024, 2048], P('tp'), may hold values from -0.125 to 0.125
Outputs:
- mixed: bfloat16 [12288, 2048], P('sp', 'tp')
The draws below stay inside these ranges and needn't reach their ends.
All inputs are finite; a program needn't handle non-finite values.
Results may differ from the reference program's by a relative error of at most 0.019.
Values may be sent and summed in bfloat16 or wider, within the bound.
A program may use at most 64 MiB of HBM per device.

```python
import jax
import jax.numpy as jnp
from jax import lax

D = 2048
HEAD_DIM = 128
RET_HEADS = 8
SB_HEADS = 8
TOK_DEV = 384
TOKENS = 12288


def draw_log_decay(key, part):
    streams = jax.random.split(key, 7)
    slow_share = 0.5
    base_rate = jax.random.uniform(streams[0], (RET_HEADS,), jnp.float32, 0.2, 0.5)
    slow_heads = jax.random.bernoulli(streams[1], slow_share, (RET_HEADS,))
    fast_rate = jax.random.uniform(streams[2], (RET_HEADS,), jnp.float32, 1.0 / 60.0, 1.0 / 30.0)
    head_decay_rate = jnp.where(slow_heads, base_rate / TOKENS, fast_rate)
    block_count = TOKENS // TOK_DEV
    block_multiplier = jnp.exp(jax.random.uniform(streams[3], (block_count, RET_HEADS), jnp.float32, -0.69, 0.69))
    block_multiplier = jnp.repeat(block_multiplier, TOK_DEV, axis=0)
    jaggedness = jnp.exp(jax.random.uniform(streams[4], (TOKENS, RET_HEADS), jnp.float32, -0.5, 0.47))
    location_list = jax.random.randint(streams[5], (2, RET_HEADS), 0, TOKENS)
    loss_values = jax.random.uniform(streams[6], (2, RET_HEADS), jnp.float32, 0.2, 0.4)
    row_position_index = jnp.arange(TOKENS, dtype=jnp.int32)[:, None]
    spike_groups = jnp.where(row_position_index == location_list[0][None, :], jnp.log(1.0 - loss_values[0])[None, :], 0.0)
    spike_groups = spike_groups + jnp.where(row_position_index == location_list[1][None, :], jnp.log(1.0 - loss_values[1])[None, :], 0.0)
    return (-head_decay_rate[None, :] * block_multiplier * jaggedness + spike_groups).astype(jnp.float32)


def draw_stick_bias(key, part):
    return jax.random.uniform(key, (SB_HEADS,), jnp.float32, -13.0, -5.0)


def block_levels(own_key, shape, pieces, smallest, high):
    def one(position, parts):
        draws = jax.random.uniform(jax.random.fold_in(jax.random.fold_in(own_key, 6), position), (parts,), jnp.float32, smallest / len(pieces), high / len(pieces))
        return jnp.repeat(jnp.exp(draws), shape[position] // parts).reshape((-1,) + (1,) * (len(shape) - position - 1))

    loudness = one(*pieces[0])
    for cut in pieces[1:]:
        loudness = loudness * one(*cut)
    return loudness


def scatter_about(key, extent, scale, bound, shards=(), kind=jnp.bfloat16):
    loudness = block_levels(key, extent, shards, -0.22, 0.18) if shards else 1.0
    entries = jax.random.normal(key, extent, jnp.float32) * scale * loudness
    return jnp.minimum(jnp.maximum(entries, -bound), bound).astype(kind)


def setup_inputs(seed: int = 0) -> dict:
    seeds = jax.random.split(jax.random.key(seed), 12)
    tokens = scatter_about(seeds[0], (TOKENS, D), 1.0, 6.0, ((0, 32), (1, 8)))
    ret_query = scatter_about(seeds[1], (D, RET_HEADS * HEAD_DIM), D ** -0.5, 0.125, ((1, 8),))
    ret_key = scatter_about(seeds[2], (D, RET_HEADS * HEAD_DIM), D ** -0.5, 0.125, ((1, 8),))
    ret_value = scatter_about(seeds[3], (D, RET_HEADS * HEAD_DIM), D ** -0.5, 0.125, ((1, 8),))
    stick_query = scatter_about(seeds[4], (D, SB_HEADS * HEAD_DIM), D ** -0.5, 0.125, ((1, 8),))
    stick_key = scatter_about(seeds[5], (D, SB_HEADS * HEAD_DIM), D ** -0.5, 0.125, ((1, 8),))
    stick_value = scatter_about(seeds[6], (D, SB_HEADS * HEAD_DIM), D ** -0.5, 0.125, ((1, 8),))
    log_decay = draw_log_decay(jax.random.fold_in(seeds[11], 71), 0)
    stick_bias = draw_stick_bias(jax.random.fold_in(seeds[11], 71), 0)
    out_ret = scatter_about(seeds[9], (RET_HEADS * HEAD_DIM, D), ((RET_HEADS + SB_HEADS) * HEAD_DIM) ** -0.5, 0.125, ((0, 8),))
    out_stick = scatter_about(seeds[10], (SB_HEADS * HEAD_DIM, D), ((RET_HEADS + SB_HEADS) * HEAD_DIM) ** -0.5, 0.125, ((0, 8),))
    return dict(tokens=tokens, ret_query=ret_query, ret_key=ret_key, ret_value=ret_value, stick_query=stick_query, stick_key=stick_key, stick_value=stick_value, log_decay=log_decay, stick_bias=stick_bias, out_ret=out_ret, out_stick=out_stick)


EPS = 1e-05
ROPE_BASE = 10000.0

def rounded(values):
    return lax.optimization_barrier(values.astype(jnp.bfloat16)).astype(jnp.float32)

def rotate(values, positions):
    half_width = values.shape[-1] // 2
    inverse = ROPE_BASE ** (-jnp.arange(half_width, dtype=jnp.float32) / half_width)
    angles = positions[:, None] * inverse[None, :]
    cosine = jnp.cos(angles)[:, None, :]
    sine_part = jnp.sin(angles)[:, None, :]
    first_half = values[..., :half_width]
    second_half = values[..., half_width:]
    return jnp.concatenate([first_half * cosine - second_half * sine_part, first_half * sine_part + second_half * cosine], axis=-1)

def head_norm(values):
    centred = values - lax.optimization_barrier(jnp.mean(values, axis=-1, keepdims=True))
    spread = lax.optimization_barrier(jnp.mean(centred * centred, axis=-1, keepdims=True))
    return centred * lax.rsqrt(spread + EPS)

def retention(query_rot, key_rot, value_rows, log_decay):
    blocks = TOKENS // TOK_DEV
    head_count = query_rot.shape[1]
    index_rows = jnp.arange(TOK_DEV, dtype=jnp.int32)
    lower = (index_rows[:, None] >= index_rows[None, :])[None]

    def split(values):
        return values.reshape((blocks, TOK_DEV) + values.shape[1:])

    def advance(state, block):
        query_block, key_block, value_block, decay_block = block
        cumulative = jnp.cumsum(decay_block, axis=0)
        final_decay = cumulative[-1]
        gaps = cumulative.T[:, :, None] - cumulative.T[:, None, :]
        decay = jnp.where(lower, jnp.exp(jnp.where(lower, gaps, 0.0)), 0.0)
        scores = jnp.einsum('thd,shd->hts', query_block.astype(jnp.float32), key_block.astype(jnp.float32))
        inner = rounded(scores * decay)
        local_part = jnp.einsum('hts,she->the', inner, value_block.astype(jnp.float32))
        carried = jnp.einsum('thd,hde->the', query_block.astype(jnp.float32), state, precision=lax.Precision.HIGHEST) * jnp.exp(cumulative)[:, :, None]
        weighted = rounded(key_block.astype(jnp.float32) * jnp.exp(final_decay[None, :] - cumulative)[:, :, None])
        fresh = jnp.einsum('shd,she->hde', weighted, value_block.astype(jnp.float32))
        state = jnp.exp(final_decay)[:, None, None] * state + fresh
        return (state, local_part + carried)
    start_state = jnp.zeros((head_count, HEAD_DIM, HEAD_DIM), jnp.float32)
    _, outputs = lax.scan(advance, start_state, (split(query_rot), split(key_rot), split(value_rows), split(log_decay)))
    return outputs.reshape(TOKENS, head_count, HEAD_DIM)

def stick_breaking(queries, keys, values, bias):
    blocks = TOKENS // TOK_DEV
    head_count = queries.shape[1]
    scale = HEAD_DIM ** (-0.5)
    keys_heads = jnp.transpose(keys, (1, 0, 2)).astype(jnp.float32)
    values_heads = jnp.transpose(values, (1, 0, 2)).astype(jnp.float32).reshape(head_count, blocks, TOK_DEV, HEAD_DIM)
    key_pos = jnp.arange(TOKENS, dtype=jnp.int32)

    def one_block(index):
        block_queries = lax.dynamic_slice_in_dim(queries, index * TOK_DEV, TOK_DEV, 0)
        query_heads = jnp.transpose(block_queries, (1, 0, 2)).astype(jnp.float32)
        query_pos = index * TOK_DEV + jnp.arange(TOK_DEV, dtype=jnp.int32)
        visible = (key_pos[None, :] < query_pos[:, None]).reshape(TOK_DEV, blocks, TOK_DEV)

        def one_head(query_h, key_h, value_h, bias_h):
            logits = (jnp.dot(query_h, key_h.T) * scale + bias_h).reshape(TOK_DEV, blocks, TOK_DEV)
            success = jax.nn.log_sigmoid(logits)
            failure = jnp.where(visible, success - logits, 0.0)
            suffix = lax.cumsum(failure, axis=2, reverse=True) - failure
            weights = rounded(jnp.where(visible, jnp.exp(success + suffix), 0.0))
            partial_value = jnp.einsum('tpk,pke->tpe', weights, value_h)
            totals = lax.optimization_barrier(jnp.sum(failure, axis=2))
            behind = lax.cumsum(totals, axis=1, reverse=True) - totals
            return lax.optimization_barrier(jnp.sum(jnp.exp(behind)[:, :, None] * partial_value, axis=1))
        return jax.vmap(one_head)(query_heads, keys_heads, values_heads, bias)
    outputs = lax.map(one_block, jnp.arange(blocks, dtype=jnp.int32))
    return jnp.transpose(outputs, (0, 2, 1, 3)).reshape(TOKENS, head_count, HEAD_DIM)

def reference(tokens, ret_query, ret_key, ret_value, stick_query, stick_key, stick_value, log_decay, stick_bias, out_ret, out_stick):

    def project(matrix):
        return jnp.dot(tokens, matrix, preferred_element_type=jnp.float32).astype(jnp.bfloat16).reshape(TOKENS, -1, HEAD_DIM)
    positions = jnp.arange(TOKENS, dtype=jnp.float32)
    query_rot = rotate(project(ret_query).astype(jnp.float32), positions).astype(jnp.bfloat16)
    key_rot = (rotate(project(ret_key).astype(jnp.float32), positions) * HEAD_DIM ** (-0.5)).astype(jnp.bfloat16)
    ret_out = head_norm(retention(query_rot, key_rot, project(ret_value), log_decay)).astype(jnp.bfloat16)
    stick_out = head_norm(stick_breaking(project(stick_query), project(stick_key), project(stick_value), stick_bias)).astype(jnp.bfloat16)
    mixed = jnp.dot(ret_out.reshape(TOKENS, -1), out_ret, preferred_element_type=jnp.float32)
    mixed = mixed + jnp.dot(stick_out.reshape(TOKENS, -1), out_stick, preferred_element_type=jnp.float32)
    return mixed.astype(jnp.bfloat16)
```

```python
import math

import jax
import jax.numpy as jnp
import numpy as np
from jax import lax
from jax.experimental import pallas as pl
from jax.experimental.pallas import tpu as pltpu
from jax.sharding import Mesh
from jax.sharding import PartitionSpec as P

HEAD_DIM = 128
ROWS = 384
HALF = ROWS // 2
D = 2048
NZ, NX, NY, NC = 8, 4, 4, 2
SP = ("z", "x")
TP = ("y", "c")
EPS = 1e-05
ROPE_BASE = 10000.0
LOG2E = math.log2(math.e)
SCALE = HEAD_DIM**-0.5
CLAMP = 120.0
MESH = pl.DeviceIdType.MESH
F32, BF16 = jnp.float32, jnp.bfloat16


def angle_tables():
    half = HEAD_DIM // 2
    inverse = ROPE_BASE ** (-np.arange(half, dtype=np.float64) / half)
    sign = np.concatenate([-np.ones(half), np.ones(half)])
    inside = np.arange(ROWS)[:, None] * np.concatenate([inverse, inverse])[None]
    start = (np.arange(NZ * NX) * ROWS)[:, None] * np.concatenate([inverse, inverse])[None]
    return tuple(
        np.asarray(t, np.float32)
        for t in (np.cos(inside), np.sin(inside) * sign, np.cos(start), np.sin(start) * sign)
    )


def head_norm(values):
    centred = values - jnp.mean(values, axis=-1, keepdims=True)
    spread = jnp.mean(centred * centred, axis=-1, keepdims=True)
    return centred * lax.rsqrt(spread + EPS)


def dot(a, b):
    return jnp.dot(a, b, preferred_element_type=F32)


def dot_t(a, b):
    return lax.dot_general(a, b, (((1,), (1,)), ((), ())), preferred_element_type=F32)


def remote(src, dst, ssem, rsem, device):
    return pltpu.make_async_remote_copy(
        src_ref=src,
        dst_ref=dst,
        send_sem=ssem,
        recv_sem=rsem,
        device_id=device,
        device_id_type=MESH,
    )


class Ring:
    def __init__(self, axis, me, view, ssem, rsem):
        self.axis, self.me, self.view, self.ssem, self.rsem = axis, me, view, ssem, rsem
        self.nxt, self.prv, self.far = (me + 1) % 4, (me + 3) % 4, (me + 2) % 4

    def copy(self, slot, half, index, to):
        ref = self.view(slot, half)
        return remote(ref, ref, self.ssem.at[index], self.rsem.at[index], {self.axis: to})

    def sends(self):
        me, n, p = self.me, self.nxt, self.prv
        return [
            self.copy(me, 0, 0, n),
            self.copy(me, 1, 3, p),
            self.copy(me, 1, 1, n),
            self.copy(me, 0, 2, p),
        ]

    def start(self):
        for c in self.sends():
            c.start()

    def landed(self, index):
        slot = (self.prv, self.prv, self.nxt, self.nxt, self.far, self.far)[index]
        return self.copy(slot, index % 2, index, self.nxt)

    def wait(self, index):
        self.landed(index).wait_recv()

    def onward(self, index):
        if index == 0:
            return self.copy(self.prv, 0, 4, self.nxt)
        return self.copy(self.nxt, 1, 5, self.prv)

    def drain(self):
        for c in self.sends() + [self.onward(0), self.onward(3)]:
            c.wait_send()


class PairRing(Ring):
    def __init__(self, y, c, view, ssem, rsem, psem, qsem):
        super().__init__("y", y, lambda s, h: view(s, h, c), ssem, rsem)
        self.c, self.view2, self.psem, self.qsem = c, view, psem, qsem

    def across(self, index, core):
        slot = (self.prv, self.prv, self.nxt, self.nxt, self.far, self.far, self.me, self.me)[index]
        ref = self.view2(slot, index % 2, core)
        return remote(ref, ref, self.psem.at[index], self.qsem.at[index], {"c": 1 - self.c})

    def begin(self):
        self.start()
        self.across(6, self.c).start()
        self.across(7, self.c).start()

    def pump(self, index):
        self.wait(index)
        if index in (0, 3):
            self.onward(index).start()
        self.across(index, self.c).start()

    def other(self, index):
        self.across(index, 1 - self.c).wait_recv()

    def finish(self):
        self.drain()
        for i in range(8):
            self.across(i, self.c).wait_send()


def exchange(axis, me, count, src, slot, ssem, rsem):
    out = []
    for i in range(1, count):
        out.append(
            remote(src, slot(me, i), ssem.at[i - 1], rsem.at[i - 1], {axis: (me + i) % count})
        )
    return out


def kernel(
    tokens,
    decays,
    bias,
    base_cos,
    base_sin,
    w0,
    w1,
    w2,
    w3,
    w4,
    w5,
    o0,
    o1,
    tab_cos,
    tab_sin,
    out,
    tok,
    wbuf,
    owbuf,
    owr,
    ows,
    tabs,
    acc,
    qall,
    kbuf,
    vbuf,
    part,
    tots,
    ttx,
    csend,
    crecv,
    fresh,
    dec,
    smsg,
    stq,
    rbuf,
    sbuf,
    rq,
    rk,
    rv,
    cums,
    local,
    tri12,
    tri0,
    lsem,
    tok_s,
    tok_r,
    ret_s,
    ret_r,
    stk_s,
    stk_r,
    q_s,
    q_r,
    z_s,
    z_r,
    x_s,
    x_r,
    s_s,
    s_r,
    ow_s,
    ow_r,
):
    z, x, y, c = (lax.axis_index(a) for a in ("z", "x", "y", "c"))
    barrier = pltpu.get_barrier_semaphore()
    peers = [{"z": (z + i) % NZ} for i in range(1, NZ)]
    peers += [{"x": (x + i) % NX} for i in range(1, NX)]
    peers += [{"c": 1 - c}]
    for i in range(1, NY):
        peers += [{"y": (y + i) % NY}, {"y": (y + i) % NY, "c": 1 - c}]
    for peer in peers:
        pl.semaphore_signal(barrier, inc=1, device_id=peer, device_id_type=MESH)

    loads = [
        pltpu.make_async_copy(w, wbuf.at[:, pl.ds(128 * i, 128)], lsem.at[i])
        for i, w in enumerate((w0, w1, w2, w3, w4, w5))
    ]
    late = [
        pltpu.make_async_copy(tab_cos, tabs.at[0], lsem.at[6]),
        pltpu.make_async_copy(tab_sin, tabs.at[1], lsem.at[7]),
        pltpu.make_async_copy(o0, owbuf.at[pl.ds(0, 128)], lsem.at[8]),
        pltpu.make_async_copy(o1, owbuf.at[pl.ds(128, 128)], lsem.at[9]),
    ]
    own_tok = pltpu.make_async_copy(
        tokens, tok.at[y, :, pl.ds(pl.multiple_of(c * 256, 256), 256)], lsem.at[10]
    )
    own_tok.start()
    for load in loads + late:
        load.start()
    own_tok.wait()
    pl.semaphore_wait(barrier, len(peers))

    def tok_view(slot, half, core):
        lanes = pl.ds(pl.multiple_of(core * 256, 256), 256)
        return tok.at[slot, pl.ds(HALF * half, HALF), lanes]

    ring = PairRing(y, c, tok_view, tok_s.at[0], tok_r.at[0], tok_s.at[1], tok_r.at[1])
    ring.begin()

    i0 = lax.broadcasted_iota(jnp.int32, (256, 384), 0)
    i1 = lax.broadcasted_iota(jnp.int32, (256, 384), 1)
    tri12[...] = ((i0 > i1) | (i1 >= 256)).astype(BF16)
    j0 = lax.broadcasted_iota(jnp.int32, (128, 256), 0)
    j1 = lax.broadcasted_iota(jnp.int32, (128, 256), 1)
    tri0[...] = ((j0 > j1) | (j1 >= 128)).astype(BF16)
    r0 = lax.broadcasted_iota(jnp.int32, (ROWS, ROWS), 0)
    r1 = lax.broadcasted_iota(jnp.int32, (ROWS, ROWS), 1)
    lower = (r0 >= r1).astype(BF16)
    wide = jnp.broadcast_to(decays[...], (ROWS, HEAD_DIM))
    hi = wide.astype(BF16)
    rest = wide - hi.astype(F32)
    mid = rest.astype(BF16)
    low = (rest - mid.astype(F32)).astype(BF16)
    cum = dot(lower, hi) + dot(lower, mid) + dot(lower, low)
    cums[...] = cum
    dec[x] = jnp.broadcast_to(cum[ROWS - 1 :, :], (8, HEAD_DIM))
    dec_out = exchange("x", x, NX, dec.at[x], lambda me, i: dec.at[me], x_s.at[0], x_r.at[0])
    for copy in dec_out:
        copy.start()

    ring.pump(0)
    ring.pump(3)
    ring.pump(1)
    ring.pump(2)
    for load in loads:
        load.wait()
    ring.other(6)
    ring.other(7)

    def project(slot):
        rows = pl.ds(pl.multiple_of(slot * 512, 512), 512)
        return dot(tok[slot], wbuf[rows, :])

    acc[...] = project(y)
    ring.pump(4)
    ring.pump(5)
    ring.other(0)
    ring.other(1)
    acc[...] += project(ring.prv)
    ring.other(2)
    ring.other(3)
    acc[...] += project(ring.nxt)
    ring.other(4)
    ring.other(5)
    acc[...] += project(ring.far)
    total = acc[...]
    qall[x] = total[:, 384:512].astype(BF16)
    kbuf[0] = total[:, 512:640].astype(BF16)
    vbuf[0] = total[:, 640:768].astype(BF16)

    zu, zd = (z + 1) % NZ, (z + NZ - 1) % NZ

    def hop(buf, which, frm, to, device):
        return remote(
            buf.at[frm], buf.at[to], z_s.at[which, to], z_r.at[which, to], {"z": device}
        )

    def up(buf, which, d):
        return hop(buf, which, d, d + 1, zu)

    def down(buf, which, d):
        return hop(buf, which, d, d - 1, zd)

    def here(buf, which, d):
        hop(buf, which, d, d, zu).wait_recv()

    up(kbuf, 0, 0).start()
    hop(kbuf, 0, 0, 7, zd).start()
    qring = Ring(
        "x", x, lambda s, h: qall.at[s, pl.ds(HALF * h, HALF)], q_s, q_r
    )
    qring.start()
    up(vbuf, 1, 0).start()
    hop(vbuf, 1, 0, 7, zd).start()
    ring.finish()

    for load in late:
        load.wait()
    sp = z * NX + x
    bc, bs = base_cos[pl.ds(sp, 1), :], base_sin[pl.ds(sp, 1), :]
    cosine = tabs[0] * bc - tabs[1] * bs
    sine = tabs[1] * bc + tabs[0] * bs

    def rotate(values):
        return values * cosine + pltpu.roll(values, HEAD_DIM // 2, 1) * sine

    qr = rotate(acc[:, 0:128].astype(BF16).astype(F32)).astype(BF16)
    kr = (rotate(acc[:, 128:256].astype(BF16).astype(F32)) * SCALE).astype(BF16)
    vr = acc[:, 256:384].astype(BF16)
    rq[...] = qr
    cum = cums[...]
    weighted = (kr.astype(F32) * jnp.exp(cum[ROWS - 1 :, :] - cum)).astype(BF16)
    rk[...] = kr
    rv[...] = vr
    fresh[x] = lax.dot_general(
        weighted, vr, (((0,), (0,)), ((), ())), preferred_element_type=F32
    ).astype(BF16)
    fresh_out = exchange(
        "x", x, NX, fresh.at[x], lambda me, i: fresh.at[me], x_s.at[1], x_r.at[1]
    )
    for copy in fresh_out:
        copy.start()

    def weight_copies():
        copies = []
        for i in range(NY):
            for other in range(2):
                if i == 0 and other == 0:
                    continue
                ty, tc = (y + i) % NY, (c + other) % 2
                columns = pl.ds(pl.multiple_of((ty * 2 + tc) * 256, 256), 256)
                rows = pl.ds(pl.multiple_of(c * 128, 128), 128)
                for m, dst in enumerate((owr, ows)):
                    copies.append(
                        remote(
                            owbuf.at[pl.ds(128 * m, 128), columns],
                            dst.at[y, rows],
                            ow_s.at[m, i, other],
                            ow_r.at[m, i, other],
                            {"y": ty, "c": tc},
                        )
                    )
        return copies

    own_rows = pl.ds(pl.multiple_of(c * 128, 128), 128)
    own_columns = pl.ds(pl.multiple_of((y * 2 + c) * 256, 256), 256)
    keep = [
        pltpu.make_async_copy(owbuf.at[pl.ds(128 * m, 128), own_columns], dst.at[y, own_rows], lsem.at[11 + m])
        for m, dst in enumerate((owr, ows))
    ]
    for copy in weight_copies() + keep:
        copy.start()

    tots[...] = jnp.zeros_like(tots)
    offset = bias[0] * LOG2E
    lanes = lax.broadcasted_iota(jnp.int32, (ROWS, HEAD_DIM), 1)

    def pair(d, xq, masked):
        scores = dot_t(qall[xq], kbuf[d])
        u = scores * (SCALE * LOG2E) + offset
        soft = jnp.maximum(jnp.log2(1.0 + jnp.exp2(jnp.minimum(u, CLAMP))), u)
        if masked:
            visible = lax.broadcasted_iota(jnp.int32, (ROWS, ROWS), 0) > (
                lax.broadcasted_iota(jnp.int32, (ROWS, ROWS), 1)
            )
            success = u - soft
            soft = jnp.where(visible, soft, 0.0)
        else:
            success = u - soft
        f = soft.astype(BF16)
        r12 = dot(f[:, 128:], tri12[...])
        rr = dot(f[:, :128], tri0[...])
        later = r12[:, 256:]
        suffix = jnp.concatenate([rr[:, :128] + later, r12[:, :256]], axis=1)
        weights = jnp.exp2(success - suffix)
        if masked:
            weights = jnp.where(visible, weights, 0.0)
        part[d, xq] = dot(weights.astype(BF16), vbuf[d])
        tots[xq] = jnp.where(lanes == d, rr[:, 128:] + later, tots[xq])

    def pairs(d):
        @pl.loop(0, NX)
        def _(xq):
            run = jnp.logical_or(
                jnp.logical_and(d > 0, d <= z), jnp.logical_and(d == 0, xq > x)
            )

            @pl.when(run)
            def _():
                pair(d, xq, False)

            @pl.when(jnp.logical_not(jnp.logical_or(run, jnp.logical_and(d == 0, xq == x))))
            def _():
                part[d, xq] = jnp.zeros((ROWS, HEAD_DIM), F32)

    pair(0, x, True)

    def local_part():
        cum = cums[...]
        row = cum.T[0:1, :]
        r0 = lax.broadcasted_iota(jnp.int32, (ROWS, ROWS), 0)
        r1 = lax.broadcasted_iota(jnp.int32, (ROWS, ROWS), 1)
        keep = r0 >= r1
        gap = jnp.concatenate([cum, cum, cum], axis=1) - row
        fade = jnp.exp(jnp.where(keep, gap, 0.0))
        inner = jnp.where(keep, dot_t(rq[...], rk[...]) * fade, 0.0).astype(BF16)
        local[...] = dot(inner, rv[...])

    local_part()
    for i in (0, 3, 1, 2):
        qring.wait(i)
        if i in (0, 3):
            qring.onward(i).start()

    quarter = pl.ds(pl.multiple_of(x * 32, 32), 32)

    def plane_sum():
        for copy in dec_out + fresh_out:
            copy.wait_recv()
        state = jnp.zeros((32, HEAD_DIM), F32)
        whole = jnp.zeros((1, HEAD_DIM), F32)
        for k in range(NX):
            own = dec[k][0:1, :]
            state = state * jnp.exp(own) + fresh[k, quarter, :].astype(F32)
            whole = whole + own
        smsg[0, 0:32, :] = state
        smsg[0, 32:40, :] = jnp.broadcast_to(whole, (8, HEAD_DIM))

    s_out = exchange("z", z, NZ, smsg.at[0], lambda me, i: smsg.at[i], s_s, s_r)

    def plane_prefix():
        for copy in s_out:
            copy.wait_recv()
        state = jnp.zeros((32, HEAD_DIM), F32)
        for d in range(NZ - 1, 0, -1):
            state = jnp.where(d <= z, state * jnp.exp(smsg[d, 32:33, :]) + smsg[d, 0:32, :], state)
        stq[x] = state

    q_out = exchange("x", x, NX, stq.at[x], lambda me, i: stq.at[me], x_s.at[2], x_r.at[2])

    def head_view(buf):
        def view(slot, half, core):
            lanes = pl.ds(pl.multiple_of(core * 128, 128), 128)
            return buf.at[slot, pl.ds(HALF * half, HALF), lanes]

        return view

    rring = PairRing(y, c, head_view(rbuf), ret_s.at[0], ret_r.at[0], ret_s.at[1], ret_r.at[1])
    sring = PairRing(y, c, head_view(sbuf), stk_s.at[0], stk_r.at[0], stk_s.at[1], stk_r.at[1])
    own_lanes = pl.ds(pl.multiple_of(c * 128, 128), 128)

    def retention_out():
        for copy in q_out:
            copy.wait_recv()
        state = jnp.concatenate([stq[k] for k in range(NX)], axis=0)
        for k in range(NX - 1):
            nxt = state * jnp.exp(dec[k][0:1, :]) + fresh[k].astype(F32)
            state = jnp.where(k < x, nxt, state)
        hi = state.astype(BF16)
        low = (state - hi.astype(F32)).astype(BF16)
        carried = (dot(rq[...], hi) + dot(rq[...], low)) * jnp.exp(cums[...])
        rbuf[y, :, own_lanes] = head_norm(local[...] + carried).astype(BF16)

    @pl.loop(1, 4)
    def _(k):
        here(kbuf, 0, k)
        up(kbuf, 0, k).start()
        here(kbuf, 0, 8 - k)

        @pl.when(k < 3)
        def _():
            down(kbuf, 0, 8 - k).start()

        @pl.when(k == 1)
        def _():
            qring.wait(4)
            qring.wait(5)

        pairs((9 - k) % 8)
        here(vbuf, 1, k)

        @pl.when(k < 3)
        def _():
            up(vbuf, 1, k).start()

        here(vbuf, 1, 8 - k)
        down(vbuf, 1, 8 - k).start()

        @pl.when(k == 1)
        def _():
            plane_sum()
            for copy in s_out:
                copy.start()

        @pl.when(k == 2)
        def _():
            plane_prefix()
            for copy in q_out:
                copy.start()

        @pl.when(k == 3)
        def _():
            retention_out()
            rring.begin()

        pairs(k)

    here(kbuf, 0, 4)
    here(vbuf, 1, 4)
    rring.pump(0)
    rring.pump(3)

    @pl.loop(0, 2)
    def _(k):
        pairs(5 - k)

    for k in range(NX):
        ttx[x, pl.ds(8 * k, 8), :] = tots[k].T[0:8, :]
    t_out = exchange("x", x, NX, ttx.at[x], lambda me, i: ttx.at[me], x_s.at[3], x_r.at[3])
    for copy in t_out:
        copy.start()
    for i in (1, 2, 4, 5):
        rring.pump(i)
    for copy in weight_copies():
        copy.wait_recv()
    for copy in keep:
        copy.wait()
    for i in (6, 7, 0, 1, 2, 3, 4, 5):
        rring.other(i)
    for copy in t_out:
        copy.wait_recv()

    c_out = []
    for i in range(1, NX):
        to = (x + i) % NX
        c_out.append(
            remote(csend.at[to], crecv.at[x], x_s.at[4, i - 1], x_r.at[4, i - 1], {"x": to})
        )

    def combine(xq):
        rows = pl.ds(pl.multiple_of(8 * xq, 8), 8)
        behind = jnp.zeros((1, ROWS), F32)
        plane = jnp.zeros((8, ROWS), F32)
        after = jnp.zeros((8, ROWS), F32)
        for k in range(NX):
            mine = ttx[k, rows, :]
            plane = plane + mine
            after = jnp.where(k > x, after + mine, after)
        lines = []
        for d in range(NZ):
            lines.append(behind + after[d : d + 1, :])
            behind = behind + plane[d : d + 1, :]
        w = jnp.exp2(-jnp.concatenate(lines, axis=0))
        w = jnp.concatenate([w, jnp.zeros((120, ROWS), F32)], axis=0).T
        value = w[:, 0:1] * part[0, xq]
        for d in range(1, NZ):
            value = value + w[:, d : d + 1] * part[d, xq]
        csend[xq] = value.astype(BF16)

    for i in range(1, NX):
        combine((x + (2, 1, 3)[i - 1]) % NX)
        c_out[(2, 1, 3)[i - 1] - 1].start()
    combine(x)
    acc[:, 0:256] = dot(rbuf[0], owr[0])
    for k in range(1, NY):
        acc[:, 0:256] += dot(rbuf[k], owr[k])
    for copy in c_out:
        copy.wait_recv()
    value = csend[x].astype(F32)
    for i in range(1, NX):
        value = value + crecv[(x + i) % NX].astype(F32)
    sbuf[y, :, own_lanes] = head_norm(value).astype(BF16)
    sring.begin()
    for i in (0, 3, 1, 2):
        sring.pump(i)
    sring.other(6)
    sring.other(7)
    acc[:, 0:256] += dot(sbuf[y], ows[y])
    sring.pump(4)
    sring.pump(5)
    sring.other(0)
    sring.other(1)
    acc[:, 0:256] += dot(sbuf[sring.prv], ows[sring.prv])
    sring.other(2)
    sring.other(3)
    acc[:, 0:256] += dot(sbuf[sring.nxt], ows[sring.nxt])
    sring.other(4)
    sring.other(5)
    out[...] = (acc[:, 0:256] + dot(sbuf[sring.far], ows[sring.far])).astype(BF16)

    qring.drain()
    rring.finish()
    sring.finish()
    for copy in dec_out + fresh_out + s_out + q_out + t_out + c_out + weight_copies():
        copy.wait_send()
    hop(kbuf, 0, 0, 7, zd).wait_send()
    hop(vbuf, 1, 0, 7, zd).wait_send()
    for d in range(0, 4):
        up(kbuf, 0, d).wait_send()
    for d in range(0, 3):
        up(vbuf, 1, d).wait_send()
    for d in (7, 6):
        down(kbuf, 0, d).wait_send()
    for d in (7, 6, 5):
        down(vbuf, 1, d).wait_send()


def body(tokens, rq, rk, rv, sq, sk, sv, log_decay, stick_bias, out_ret, out_stick):
    ct, st, cb, sb = (jnp.asarray(t) for t in angle_tables())
    vmem = pl.BlockSpec(memory_space=pltpu.VMEM)
    anym = pl.BlockSpec(memory_space=pl.ANY)
    smem = pl.BlockSpec(memory_space=pltpu.SMEM)
    v, dma = pltpu.VMEM, pltpu.SemaphoreType.DMA
    return pl.pallas_call(
        kernel,
        out_shape=jax.ShapeDtypeStruct((ROWS, 256), BF16),
        in_specs=[anym, vmem, smem, vmem, vmem] + [anym] * 10,
        out_specs=vmem,
        scratch_shapes=[
            v((NY, ROWS, 512), BF16),
            v((D, 768), BF16),
            v((256, D), BF16),
            v((NY, 256, 256), BF16),
            v((NY, 256, 256), BF16),
            v((2, ROWS, HEAD_DIM), F32),
            v((ROWS, 768), F32),
            v((NX, ROWS, HEAD_DIM), BF16),
            v((NZ, ROWS, HEAD_DIM), BF16),
            v((NZ, ROWS, HEAD_DIM), BF16),
            v((NZ, NX, ROWS, HEAD_DIM), F32),
            v((NX, ROWS, HEAD_DIM), F32),
            v((NX, 32, ROWS), F32),
            v((NX, ROWS, HEAD_DIM), BF16),
            v((NX, ROWS, HEAD_DIM), BF16),
            v((NX, HEAD_DIM, HEAD_DIM), BF16),
            v((NX, 8, HEAD_DIM), F32),
            v((NZ, 40, HEAD_DIM), F32),
            v((NX, 32, HEAD_DIM), F32),
            v((NY, ROWS, 256), BF16),
            v((NY, ROWS, 256), BF16),
            v((ROWS, HEAD_DIM), BF16),
            v((ROWS, HEAD_DIM), BF16),
            v((ROWS, HEAD_DIM), BF16),
            v((ROWS, HEAD_DIM), F32),
            v((ROWS, HEAD_DIM), F32),
            v((256, 384), BF16),
            v((128, 256), BF16),
            dma((13,)),
            dma((2, 8)),
            dma((2, 8)),
            dma((2, 8)),
            dma((2, 8)),
            dma((2, 8)),
            dma((2, 8)),
            dma((6,)),
            dma((6,)),
            dma((2, 8)),
            dma((2, 8)),
            dma((5, 3)),
            dma((5, 3)),
            dma((7,)),
            dma((7,)),
            dma((2, NY, 2)),
            dma((2, NY, 2)),
        ],
        compiler_params=pltpu.CompilerParams(
            collective_id=0, has_side_effects=True, vmem_limit_bytes=48 * 1024 * 1024
        ),
    )(
        tokens,
        log_decay,
        stick_bias,
        cb,
        sb,
        rq,
        rk,
        rv,
        sq,
        sk,
        sv,
        out_ret,
        out_stick,
        ct,
        st,
    )


def solution(mesh):
    grid = Mesh(mesh.devices.reshape(NZ, NX, NY, NC), ("z", "x", "y", "c"))
    return jax.shard_map(
        body,
        mesh=grid,
        in_specs=(
            P(SP, TP),
            P(None, TP),
            P(None, TP),
            P(None, TP),
            P(None, TP),
            P(None, TP),
            P(None, TP),
            P(SP, TP),
            P(TP),
            P(TP, None),
            P(TP, None),
        ),
        out_specs=P(SP, TP),
        check_vma=False,
    )
```
